512 devices in a mesh: kv: 64 (over z, y), tp: 8 (over x, core).
Axes of the slice: x: 4, y: 8, z: 8, core: 2. Of those that a mesh axis runs over, the one named last changes fastest.
Arguments:
- hidden_in: bfloat16 [256, 2048], P('tp', 'kv'), may hold values from -20 to 20
- gain_before: float32 [2048], P('kv'), may hold values from 0.1 to 1.9
- gate_before: bfloat16 [2048, 5632], P('kv', 'tp'), may hold values from -0.125 to 0.125
- lift_before: bfloat16 [2048, 5632], P('kv', 'tp'), may hold values from -0.125 to 0.125
- drop_before: bfloat16 [5632, 2048], P('tp', 'kv'), may hold values from -0.078125 to 0.078125
- mixer_gain: float32 [2048], P('kv'), may hold values from 0.1 to 1.9
- value_proj: bfloat16 [2048, 2048], P('kv', 'tp'), may hold values from -0.125 to 0.125
- gate_proj: bfloat16 [2048, 2048], P('kv', 'tp'), may hold values from -0.125 to 0.125
- key_proj: bfloat16 [2048, 1024], P('kv', 'tp'), may hold values from -0.125 to 0.125
- query_proj: bfloat16 [2048, 1024], P('kv', 'tp'), may hold values from -0.125 to 0.125
- step_proj: bfloat16 [2048, 32], P('kv'), may hold values from -0.125 to 0.125
- value_taps: float32 [4, 2048], P(None, 'tp'), may hold values from -3 to 3
- key_taps: float32 [4, 1024], P(None, 'tp'), may hold values from -3 to 3
- query_taps: float32 [4, 1024], P(None, 'tp'), may hold values from -3 to 3
- value_past: bfloat16 [256, 3, 2048], P('kv', None, 'tp'), may hold values from -6 to 6
- key_past: bfloat16 [256, 3, 1024], P('kv', None, 'tp'), may hold values from -6 to 6
- query_past: bfloat16 [256, 3, 1024], P('kv', None, 'tp'), may hold values from -6 to 6
- decay_rate: float32 [32], P('tp'), may hold values from 0.05 to 1
- block_state: float32 [256, 32, 64, 128], P('kv', 'tp'), may hold values from -24 to 24
- block_keys: bfloat16 [256, 128, 1024], P('kv', None, 'tp'), may hold values from -6 to 6
- block_values: bfloat16 [256, 128, 2048], P('kv', None, 'tp'), may hold values from -6 to 6
- block_steps: float32 [256, 128, 32], P('kv', None, 'tp'), may hold values from 0.2 to 2
- block_decay: float32 [256, 128, 32], P('kv', None, 'tp'), may hold values from -1.25 to 0
- lengths: int32 [256], P('kv'), may hold values from 1 to 128, 8192 in all
- head_gain: float32 [2048], P('tp'), may hold values from 0.1 to 1.9
- out_proj: bfloat16 [2048, 2048], P('tp', 'kv'), may hold values from -0.125 to 0.125
- gain_after: float32 [2048], P('kv'), may hold values from 0.1 to 1.9
- gate_after: bfloat16 [2048, 5632], P('kv', 'tp'), may hold values from -0.125 to 0.125
- lift_after: bfloat16 [2048, 5632], P('kv', 'tp'), may hold values from -0.125 to 0.125
- drop_after: bfloat16 [5632, 2048], P('tp', 'kv'), may hold values from -0.078125 to 0.078125
Outputs:
- hidden_out: bfloat16 [256, 2048], P('tp', 'kv')
The draws below stay inside these ranges and needn't reach their ends.
Inputs may be any that keep to these rules, and one draw needn't show every extreme that they name: `lengths`: some sequence has all 128 positions filled.
All inputs are finite; a program needn't handle non-finite values. No bound on the sum of `lengths` on one device may be relied on, other than what follows from the above.
Results may differ from the reference program's by a relative error of at most 0.014.
Values may be sent and summed in bfloat16 or wider, within the bound.
A program may use at most 64 MiB of HBM per device.

```python
import math
import jax
import jax.numpy as jnp
import numpy as np
from jax import lax

D = 2048
FF = 5632
HEAD_DIM = 64
STATE = 128
GROUPS = 8
BLOCK_POSITIONS = 128
CONV = 4
HEADS = 32
SEQUENCE_TOTAL = 256
N_TP = 8


def draw_hidden_in(key, part):
    first_key = jax.random.fold_in(jax.random.fold_in(key, 11), 0)
    column = jnp.arange(D, dtype=jnp.float32) / D
    draws = jnp.clip(jax.random.normal(first_key, (SEQUENCE_TOTAL, D), jnp.float32), -6.0, 6.0)
    values = draws * jnp.exp(column * jnp.log(3.0))[None, :]
    return values.astype(jnp.bfloat16)


def draw_block_decay(key, part):
    random_key_table = jax.random.split(jax.random.fold_in(key, 23), 7)
    fast_share = 0.5
    fast_heads = jax.random.uniform(random_key_table[0], (HEADS,), jnp.float32) < fast_share
    fast_rate = jax.random.uniform(random_key_table[1], (HEADS,), jnp.float32, 2.5, 4.5) / BLOCK_POSITIONS
    slow_rate = jax.random.uniform(random_key_table[2], (HEADS,), jnp.float32, 0.2, 1.0) / BLOCK_POSITIONS
    head_rate = jnp.where(fast_heads, fast_rate, slow_rate)
    seq_factor = jnp.exp(jax.random.uniform(random_key_table[3], (SEQUENCE_TOTAL, 1, 1), jnp.float32, jnp.log(0.6), jnp.log(1.4)))
    jitter = jax.random.uniform(random_key_table[4], (SEQUENCE_TOTAL, BLOCK_POSITIONS, HEADS), jnp.float32, 0.5, 1.5)
    position_within_block = jax.random.randint(random_key_table[5], (SEQUENCE_TOTAL, 2), 0, BLOCK_POSITIONS)
    token_position = jnp.arange(BLOCK_POSITIONS, dtype=jnp.int32)
    matched_mask = jnp.any(token_position[None, :, None] == position_within_block[:, None, :], axis=2)
    keep_share = jax.random.uniform(random_key_table[6], (SEQUENCE_TOTAL, BLOCK_POSITIONS, HEADS), jnp.float32, 0.55, 0.8)
    values = -head_rate[None, None, :] * seq_factor * jitter + jnp.where(matched_mask[:, :, None], jnp.log(keep_share), 0.0)
    return values.astype(jnp.float32)


def block_levels(stream_key, shape, cuts, least, high):
    level, own = 1.0, jax.random.fold_in(stream_key, 6)
    for dim, blocks in cuts:
        steps = jnp.exp(jax.random.uniform(jax.random.fold_in(own, dim), (blocks,), jnp.float32, least / len(cuts), high / len(cuts)))
        level = level * jnp.repeat(steps, shape[dim] // blocks).reshape([-1 if axis == dim else 1 for axis in range(len(shape))])
    return level


def profile(number_of, total, limit, slope):
    weights = [(1 << 20) // math.isqrt(grade ** slope) + 1 for grade in range(2, number_of + 1)]
    spare, given = total - limit - (number_of - 1), [1] * (number_of - 1)
    while spare > 0:
        free = [i for i in range(number_of - 1) if given[i] < limit]
        whole, budget = sum([weights[i] for i in free]), spare
        for i in free:
            more = min(limit - given[i], max(1, budget * weights[i] // whole), spare)
            given[i] = given[i] + more
            spare = spare - more
    return np.array([limit] + given)


def uneven(key, number_of, total, limit, skew):
    if number_of == 2:
        one = jax.random.randint(key, (), max(1, total - limit), min(limit, total - 1) + 1)
        return jnp.stack([one, total - one])
    sizes = jnp.asarray(profile(number_of, total, limit, skew), jnp.int32)
    pairs = (number_of - 1) // 2
    donor, sink = sizes[1:1 + 2 * pairs:2], sizes[2:2 + 2 * pairs:2]
    margin = jnp.minimum(donor - 1, limit - sink)
    shifted = jax.random.randint(jax.random.fold_in(key, 1), (pairs,), 0, 1 << 20) % (margin + 1)
    sizes = sizes.at[1:1 + 2 * pairs:2].set(donor - shifted).at[2:2 + 2 * pairs:2].set(sink + shifted)
    return sizes[jax.random.permutation(jax.random.fold_in(key, 2), number_of)]


def scatter_about(stream_key, shape, deviation, most, cuts=(), kind=jnp.bfloat16):
    array = jax.random.normal(stream_key, shape, jnp.float32) * deviation
    if len(cuts) > 0:
        array = block_levels(stream_key, shape, cuts, -0.22, 0.18) * array
    return jnp.clip(array, min=-most, max=most).astype(kind)


def setup_inputs(seed: int = 0) -> dict:
    keys = jax.random.split(jax.random.key(seed), 31)
    return {
        "hidden_in": draw_hidden_in(jax.random.fold_in(keys[30], 71), 0),
        "gain_before": jnp.clip(1.0 + 0.18 * jax.random.normal(keys[1], (D,), jnp.float32), 0.1, 1.9),
        "gate_before": scatter_about(keys[2], (D, FF), D ** -0.5, 0.125, ((0, 64), (1, 8))),
        "lift_before": scatter_about(keys[3], (D, FF), D ** -0.5, 0.125, ((0, 64), (1, 8))),
        "drop_before": scatter_about(keys[4], (FF, D), FF ** -0.5, 0.078125, ((0, 8), (1, 64))),
        "mixer_gain": jnp.clip(1.0 + 0.18 * jax.random.normal(keys[5], (D,), jnp.float32), 0.1, 1.9),
        "value_proj": scatter_about(keys[6], (D, D), D ** -0.5, 0.125, ((0, 64), (1, 8))),
        "gate_proj": scatter_about(keys[7], (D, D), D ** -0.5, 0.125, ((0, 64), (1, 8))),
        "key_proj": scatter_about(keys[8], (D, GROUPS * STATE), D ** -0.5, 0.125, ((0, 64), (1, 8))),
        "query_proj": scatter_about(keys[9], (D, GROUPS * STATE), D ** -0.5, 0.125, ((0, 64), (1, 8))),
        "step_proj": scatter_about(keys[10], (D, HEADS), D ** -0.5, 0.125, ((0, 64),)),
        "value_taps": scatter_about(keys[11], (CONV, D), 0.5, 3.0, ((1, 8),), jnp.float32),
        "key_taps": scatter_about(keys[12], (CONV, GROUPS * STATE), 0.5, 3.0, ((1, 8),), jnp.float32),
        "query_taps": scatter_about(keys[13], (CONV, GROUPS * STATE), 0.5, 3.0, ((1, 8),), jnp.float32),
        "value_past": scatter_about(keys[14], (SEQUENCE_TOTAL, CONV - 1, D), 1.0, 6.0, ((0, 64), (2, 8))),
        "key_past": scatter_about(keys[15], (SEQUENCE_TOTAL, CONV - 1, GROUPS * STATE), 1.0, 6.0, ((0, 64), (2, 8))),
        "query_past": scatter_about(keys[16], (SEQUENCE_TOTAL, CONV - 1, GROUPS * STATE), 1.0, 6.0, ((0, 64), (2, 8))),
        "decay_rate": jnp.clip(jnp.exp(math.log(1.0) - 2.9957323 * jax.random.uniform(keys[17], (HEADS,), jnp.float32) ** block_levels(keys[17], (HEADS,), ((0, 8),), -0.2, 0.2)), 0.05, 1.0),
        "block_state": scatter_about(keys[18], (SEQUENCE_TOTAL, HEADS, HEAD_DIM, STATE), 4.0, 24.0, ((0, 64), (1, 8)), jnp.float32),
        "block_keys": scatter_about(keys[19], (SEQUENCE_TOTAL, BLOCK_POSITIONS, GROUPS * STATE), 1.0, 6.0, ((0, 64), (2, 8))),
        "block_values": scatter_about(keys[20], (SEQUENCE_TOTAL, BLOCK_POSITIONS, D), 1.0, 6.0, ((0, 64), (2, 8))),
        "block_steps": jnp.clip(jnp.exp(math.log(2.0) - 2.3025851 * jax.random.uniform(keys[21], (SEQUENCE_TOTAL, BLOCK_POSITIONS, HEADS), jnp.float32) ** block_levels(keys[21], (SEQUENCE_TOTAL, BLOCK_POSITIONS, HEADS), ((0, 64), (2, 8)), -0.2, 0.2)), 0.2, 2.0),
        "block_decay": draw_block_decay(jax.random.fold_in(keys[30], 71), 0),
        "lengths": uneven(keys[23], SEQUENCE_TOTAL, SEQUENCE_TOTAL * BLOCK_POSITIONS // 4, BLOCK_POSITIONS, 2).astype(jnp.int32),
        "head_gain": jnp.clip(1.0 + 0.18 * jax.random.normal(keys[24], (D,), jnp.float32), 0.1, 1.9),
        "out_proj": scatter_about(keys[25], (D, D), D ** -0.5, 0.125, ((0, 8), (1, 64))),
        "gain_after": jnp.clip(1.0 + 0.18 * jax.random.normal(keys[26], (D,), jnp.float32), 0.1, 1.9),
        "gate_after": scatter_about(keys[27], (D, FF), D ** -0.5, 0.125, ((0, 64), (1, 8))),
        "lift_after": scatter_about(keys[28], (D, FF), D ** -0.5, 0.125, ((0, 64), (1, 8))),
        "drop_after": scatter_about(keys[29], (FF, D), FF ** -0.5, 0.078125, ((0, 8), (1, 64))),
    }


EPSILON = 1e-06

def inverse_rms(rows_in):
    values = rows_in.astype(jnp.float32)
    return lax.rsqrt(lax.optimization_barrier(jnp.mean(values * values, axis=1)) + EPSILON)[:, None]

def blocked_down(hidden, weight):
    inner = hidden.shape[1] // N_TP
    hidden_blocks = hidden.reshape(hidden.shape[0], N_TP, inner).astype(jnp.float32)
    weight_blocks = weight.reshape(N_TP, inner, weight.shape[1]).astype(jnp.float32)
    pieces = jnp.einsum('btf,tfd->tbd', hidden_blocks, weight_blocks, precision=lax.Precision.HIGHEST).astype(jnp.bfloat16)
    return lax.optimization_barrier(jnp.sum(pieces.astype(jnp.float32), axis=0))

def half_mlp(rows_in, gain_vec, gate_weight, lift_weight, drop_weight):
    row_scale = inverse_rms(rows_in)
    scaled = (rows_in.astype(jnp.float32) * gain_vec[None, :]).astype(jnp.bfloat16)
    gate_vals = row_scale * jnp.dot(scaled, gate_weight, preferred_element_type=jnp.float32)
    lift_vals = row_scale * jnp.dot(scaled, lift_weight, preferred_element_type=jnp.float32)
    hidden = (jax.nn.silu(gate_vals) * lift_vals).astype(jnp.bfloat16)
    return blocked_down(hidden, drop_weight)

def convolve(past_rows, taps, newest):
    earlier = lax.optimization_barrier(jnp.sum(past_rows.astype(jnp.float32) * taps[None, :-1, :], axis=1))
    return jax.nn.silu(earlier + taps[-1][None, :] * newest)

def mixer(rows_in, mixer_gain, value_proj, gate_proj, key_proj, query_proj, step_proj, value_taps, key_taps, query_taps, value_past, key_past, query_past, decay_rate, block_state, block_keys, block_values, block_steps, block_decay, lengths, head_gain, out_proj):
    row_scale = inverse_rms(rows_in)
    scaled = (rows_in.astype(jnp.float32) * mixer_gain[None, :]).astype(jnp.bfloat16)

    def project(weight):
        return row_scale * jnp.dot(scaled, weight, preferred_element_type=jnp.float32)
    new_value = convolve(value_past, value_taps, project(value_proj))
    gate_vals = project(gate_proj)
    new_key = convolve(key_past, key_taps, project(key_proj))
    new_query = convolve(query_past, query_taps, project(query_proj))
    step_size = jax.nn.softplus(project(step_proj))
    new_decay = -decay_rate[None, :] * step_size
    batch = rows_in.shape[0]
    block_len = block_keys.shape[1]
    per_group = HEADS // GROUPS
    live_mask = (jnp.arange(block_len, dtype=jnp.int32)[None, :] < (lengths - 1)[:, None])[:, :, None]
    masked = jnp.where(live_mask, block_decay, 0.0)
    running = jnp.cumsum(masked, axis=1)
    block_total = running[:, -1, :]
    tail_sum = block_total[:, None, :] - running
    query_round = new_query.astype(jnp.bfloat16).astype(jnp.float32)
    scores = jnp.einsum('blgn,bgn->blg', block_keys.reshape(batch, block_len, GROUPS, STATE).astype(jnp.float32), query_round.reshape(batch, GROUPS, STATE), precision=lax.Precision.HIGHEST)
    scores = jnp.repeat(scores, per_group, axis=2)
    weights = jnp.where(live_mask, jnp.exp(tail_sum + new_decay[:, None, :]) * block_steps * scores, 0.0).astype(jnp.bfloat16)
    from_block = jnp.einsum('blh,blhp->bhp', weights.astype(jnp.float32), block_values.reshape(batch, block_len, HEADS, HEAD_DIM).astype(jnp.float32), precision=lax.Precision.HIGHEST)
    query_heads = jnp.repeat(new_query.reshape(batch, GROUPS, STATE), per_group, axis=1)
    source_state = jnp.einsum('bhpn,bhn->bhp', block_state, query_heads, precision=lax.Precision.HIGHEST)
    source_state = source_state * jnp.exp(block_total + new_decay)[:, :, None]
    self_score = jnp.repeat(lax.optimization_barrier(jnp.sum((new_query * new_key).reshape(batch, GROUPS, STATE), axis=2)), per_group, axis=1)
    from_token = (step_size * self_score)[:, :, None] * new_value.reshape(batch, HEADS, HEAD_DIM)
    gated_out = (source_state + from_block + from_token) * jax.nn.silu(gate_vals.reshape(batch, HEADS, HEAD_DIM))
    normed = gated_out * lax.rsqrt(lax.optimization_barrier(jnp.mean(gated_out * gated_out, axis=2, keepdims=True)) + EPSILON)
    normed = normed * head_gain.reshape(HEADS, HEAD_DIM)[None]
    mixed_rows = normed.reshape(batch, HEADS * HEAD_DIM).astype(jnp.bfloat16)
    return blocked_down(mixed_rows, out_proj)

def reference(hidden_in, gain_before, gate_before, lift_before, drop_before, mixer_gain, value_proj, gate_proj, key_proj, query_proj, step_proj, value_taps, key_taps, query_taps, value_past, key_past, query_past, decay_rate, block_state, block_keys, block_values, block_steps, block_decay, lengths, head_gain, out_proj, gain_after, gate_after, lift_after, drop_after):
    section_one = (hidden_in.astype(jnp.float32) + 0.5 * half_mlp(hidden_in, gain_before, gate_before, lift_before, drop_before)).astype(jnp.bfloat16)
    branch_mix = mixer(section_one, mixer_gain, value_proj, gate_proj, key_proj, query_proj, step_proj, value_taps, key_taps, query_taps, value_past, key_past, query_past, decay_rate, block_state, block_keys, block_values, block_steps, block_decay, lengths, head_gain, out_proj)
    section_two = (section_one.astype(jnp.float32) + branch_mix).astype(jnp.bfloat16)
    return (section_two.astype(jnp.float32) + 0.5 * half_mlp(section_two, gain_after, gate_after, lift_after, drop_after)).astype(jnp.bfloat16)
```

```python
import jax
import jax.numpy as jnp
from jax import lax
from jax.experimental import pallas as pl
from jax.experimental.pallas import tpu as pltpu
from jax.sharding import Mesh
from jax.sharding import PartitionSpec as P

D = 2048
N = 8
ROWS = 32
OWN = 4
HID = 704
HIDP = 768
MIXW = 896
STEP_AT = 768
EPSILON = 1e-06
MESH = pl.DeviceIdType.MESH
F32 = jnp.float32
BF16 = jnp.bfloat16
HIGHEST = lax.Precision.HIGHEST


def at(z, y, t):
    return (z, y, t)


def plus(a, b):
    return lax.rem(a + b, N)


def dot_nt(a, b, precision=None):
    return lax.dot_general(
        a, b, (((1,), (1,)), ((), ())), precision=precision, preferred_element_type=F32
    )


def lanes(shape):
    return lax.broadcasted_iota(jnp.int32, shape, 1)


def silu(a):
    return a / (1.0 + jnp.exp(-a))


def softplus(a):
    return jnp.maximum(a, 0.0) + jnp.log1p(jnp.exp(-jnp.abs(a)))


class Ring:
    def __init__(self, buf, ahead, back, recv, me):
        self.buf, self.ahead, self.back, self.recv = buf, ahead, back, recv
        self.z, self.y, self.t = me

    def copy(self, slot, step, forward):
        to = plus(self.z, 1 if forward else N - 1)
        return pltpu.make_async_remote_copy(
            src_ref=self.buf.at[slot],
            dst_ref=self.buf.at[slot],
            send_sem=(self.ahead if forward else self.back).at[step],
            recv_sem=self.recv.at[slot],
            device_id=at(to, self.y, self.t),
            device_id_type=MESH,
        )

    def start(self):
        self.copy(self.z, 0, True).start()
        self.copy(self.z, 0, False).start()

    def arrived(self, slot):
        self.copy(slot, 0, True).wait_recv()

    def relay(self, k):
        slot = plus(self.z, N - k)
        self.arrived(slot)
        self.copy(slot, k, True).start()
        if k <= 2:
            slot = plus(self.z, k)
            self.arrived(slot)
            self.copy(slot, k, False).start()

    def finish(self):
        self.arrived(plus(self.z, N - 4))
        self.arrived(plus(self.z, 3))

    def drain(self):
        for k in range(4):
            self.copy(self.z, k, True).wait_send()
        for k in range(3):
            self.copy(self.z, k, False).wait_send()


class Group:
    def __init__(self, src, dst, send, recv, me, axis, scatter):
        self.src, self.dst, self.send, self.recv = src, dst, send, recv
        self.me, self.axis, self.scatter = me, axis, scatter
        self.own = me[axis]

    def copy(self, d):
        to = plus(self.own, d)
        target = list(self.me)
        target[self.axis] = to
        return pltpu.make_async_remote_copy(
            src_ref=self.src.at[to] if self.scatter else self.src.at[self.own],
            dst_ref=self.dst.at[self.own],
            send_sem=self.send.at[d],
            recv_sem=self.recv.at[self.own],
            device_id=tuple(target),
            device_id_type=MESH,
        )

    def start(self):
        def body(d, c):
            self.copy(d).start()
            return c

        lax.fori_loop(1, N, body, 0)

    def wait(self):
        def body(d, c):
            slot = plus(self.own, d)
            pltpu.make_async_remote_copy(
                src_ref=self.dst.at[slot],
                dst_ref=self.dst.at[slot],
                send_sem=self.send.at[d],
                recv_sem=self.recv.at[slot],
                device_id=self.me,
                device_id_type=MESH,
            ).wait_recv()
            return c

        lax.fori_loop(1, N, body, 0)

    def drain(self):
        def body(d, c):
            self.copy(d).wait_send()
            return c

        lax.fori_loop(1, N, body, 0)


def total(ref):
    acc = ref[0].astype(F32)
    for k in range(1, N):
        acc = acc + ref[k].astype(F32)
    return acc


def stacked(ref):
    return jnp.concatenate([ref[k].astype(F32) for k in range(N)], axis=0).astype(BF16)


def spread(blocks):
    halves = []
    for half in range(2):
        acc = blocks[4 * half]
        for k in range(1, 4):
            acc = acc + pltpu.roll(blocks[4 * half + k], 32 * k, 1)
        halves.append(acc)
    return jnp.concatenate(halves, axis=1)


def piece(values, k):
    half = values[:, 128 * (k // 4) : 128 * (k // 4) + 128]
    return half if k % 4 == 0 else pltpu.roll(half, 128 - 32 * (k % 4), 1)


def with_squares(part, values, at_lane):
    squares = jnp.sum(values * values, axis=1, keepdims=True)
    high = squares.astype(BF16).astype(F32)
    low = squares - high
    lane = lanes(part.shape)
    return jnp.where(lane == at_lane, high, jnp.where(lane == at_lane + 1, low, part))


def row_scale(summed, at_lane):
    squares = summed[:, at_lane : at_lane + 1] + summed[:, at_lane + 1 : at_lane + 2]
    return lax.rsqrt(squares / D + EPSILON)


def kernel(
    x_ref,
    gains_ref,
    gate1_ref,
    lift1_ref,
    drop1_ref,
    value_proj_ref,
    gate_proj_ref,
    key_proj_ref,
    query_proj_ref,
    step_proj_ref,
    value_taps_ref,
    key_taps_ref,
    query_taps_ref,
    value_past_ref,
    key_past_ref,
    query_past_ref,
    rate_ref,
    state_ref,
    keys_ref,
    values_ref,
    steps_ref,
    decay_ref,
    lengths_ref,
    head_gain_ref,
    out_proj_ref,
    gate2_ref,
    lift2_ref,
    drop2_ref,
    out_ref,
    x_own,
    x_all,
    gains_all,
    gate1_all,
    lift1_all,
    drop1_all,
    mix_all,
    proj_all,
    gate2_all,
    lift2_all,
    drop2_all,
    rs1_src,
    rs1_dst,
    h1_all,
    sum1_all,
    rsm_src,
    rsm_dst,
    hm_all,
    summ_all,
    rs2_src,
    rs2_dst,
    h2_all,
    two_src,
    two_dst,
    end_src,
    end_dst,
    ring_ahead,
    ring_back,
    ring_recv,
    group_send,
    group_recv,
    x_send,
    x_recv,
    end_send,
    end_recv,
    two_send,
    two_recv,
):
    z = lax.axis_index("z")
    y = lax.axis_index("y")
    t = lax.axis_index("t")
    me = (z, y, t)
    diagonal = z == t

    barrier = pltpu.get_barrier_semaphore()

    def hello(target):
        pl.semaphore_signal(barrier, inc=1, device_id=target, device_id_type=MESH)

    hello(at(plus(z, 1), y, t))
    hello(at(plus(z, N - 1), y, t))

    def greet(d, c):
        hello(at(z, plus(y, d), t))
        hello(at(z, y, plus(t, d)))
        hello(at(plus(z, d), y, z))
        hello(at(t, y, plus(t, d)))
        return c

    lax.fori_loop(1, N, greet, 0)

    @pl.when(jnp.logical_not(diagonal))
    def _():
        hello(at(z, y, z))
        hello(at(t, y, t))

    rings = {}
    for k, (name, buf) in enumerate(
        (
            ("gains", gains_all),
            ("gate1", gate1_all),
            ("lift1", lift1_all),
            ("drop1", drop1_all),
            ("mix", mix_all),
            ("proj", proj_all),
            ("gate2", gate2_all),
            ("lift2", lift2_all),
            ("drop2", drop2_all),
        )
    ):
        rings[name] = Ring(buf, ring_ahead.at[k], ring_back.at[k], ring_recv.at[k], me)

    groups = []

    def group(src, dst, axis, scatter):
        k = len(groups)
        groups.append(Group(src, dst, group_send.at[k], group_recv.at[k], me, axis, scatter))
        return groups[-1]

    eye = (
        lax.broadcasted_iota(jnp.int32, (ROWS, ROWS), 0) == lanes((ROWS, ROWS))
    ).astype(F32).astype(BF16)

    def pack_wide(buf, ref):
        buf[z, :, HID:HIDP] = jnp.zeros((ROWS, HIDP - HID), BF16)
        buf[z, :, 0:HID] = ref[...]

    def pack_drop(buf, ref):
        buf[z, :, HID:HIDP] = jnp.zeros((ROWS, HIDP - HID), BF16)
        buf[z, :, 0:HID] = dot_nt(eye, ref[...]).astype(BF16)

    x_own[...] = jnp.zeros((ROWS, 128), BF16)
    x_own[:, 0:32] = x_ref[...]
    gains_all[z] = gains_ref[...]
    pack_wide(gate1_all, gate1_ref)
    pack_wide(lift1_all, lift1_ref)
    pack_drop(drop1_all, drop1_ref)
    mix_all[z, :, 0:256] = value_proj_ref[...]
    mix_all[z, :, 256:512] = gate_proj_ref[...]
    mix_all[z, :, 512:640] = key_proj_ref[...]
    mix_all[z, :, 640:768] = query_proj_ref[...]
    mix_all[z, :, 768:896] = jnp.zeros((ROWS, 128), BF16)
    mix_all[z, :, 768:800] = step_proj_ref[...]
    proj_all[z] = dot_nt(eye, out_proj_ref[...]).astype(BF16)
    pack_wide(gate2_all, gate2_ref)
    pack_wide(lift2_all, lift2_ref)
    pack_drop(drop2_all, drop2_ref)

    pl.semaphore_wait(barrier, 32 - 2 * diagonal.astype(jnp.int32))

    def x_copy(d):
        return pltpu.make_async_remote_copy(
            src_ref=x_own,
            dst_ref=x_all.at[z],
            send_sem=x_send.at[d],
            recv_sem=x_recv.at[z],
            device_id=at(t, y, plus(t, d)),
            device_id_type=MESH,
        )

    def x_start(d, c):
        x_copy(d).start()
        return c

    lax.fori_loop(1, N, x_start, 0)

    @pl.when(jnp.logical_not(diagonal))
    def _():
        x_copy(0).start()

    @pl.when(diagonal)
    def _():
        x_all[z] = x_own[...]

    rings["gains"].start()
    rings["gate1"].start()
    rings["lift1"].start()
    rings["drop1"].start()

    for k in range(1, 4):
        rings["gains"].relay(k)
        rings["gate1"].relay(k)
        rings["lift1"].relay(k)

    rings["mix"].start()
    rings["proj"].start()
    rings["drop1"].relay(1)

    def x_wait(k):
        return pltpu.make_async_remote_copy(
            src_ref=x_all.at[k],
            dst_ref=x_all.at[k],
            send_sem=x_send.at[0],
            recv_sem=x_recv.at[k],
            device_id=me,
            device_id_type=MESH,
        )

    def x_arrived(d, c):
        x_wait(plus(z, d)).wait_recv()
        return c

    lax.fori_loop(1, N, x_arrived, 0)

    @pl.when(jnp.logical_not(diagonal))
    def _():
        x_wait(z).wait_recv()

    rings["gains"].finish()
    gains = spread([gains_all[k] for k in range(N)])
    section = spread([x_all[k].astype(F32) for k in range(N)])

    def unit_open(section, gain, gate_all, lift_all, rs_src, rs_dst):
        scaled = (section * gain).astype(BF16)
        gate = jnp.dot(scaled, gate_all[...].reshape(256, HIDP), preferred_element_type=F32)
        gate = with_squares(gate, section, HID)
        lift = jnp.dot(scaled, lift_all[...].reshape(256, HIDP), preferred_element_type=F32)
        for k in range(N):
            rs_src[k, :, 0:HIDP] = gate[OWN * k : OWN * k + OWN].astype(BF16)
            rs_src[k, :, HIDP:] = lift[OWN * k : OWN * k + OWN].astype(BF16)
        exchange = group(rs_src, rs_dst, 1, True)
        exchange.start()
        rs_dst[y] = rs_src[y]
        return exchange

    def unit_hidden(exchange, rs_dst, h_all):
        exchange.wait()
        summed = total(rs_dst)
        scale = row_scale(summed, HID)
        hidden = silu(summed[:, 0:HIDP] * scale) * (summed[:, HIDP:] * scale)
        h_all[y] = hidden.astype(BF16)
        gather = group(h_all, h_all, 1, False)
        gather.start()
        return gather

    def down(gather, h_all, weight_all, width):
        gather.wait()
        return dot_nt(stacked(h_all), weight_all[...].reshape(256, width))

    def share(part, sum_all):
        sum_all[t] = part.astype(BF16)
        shared = group(sum_all, sum_all, 2, False)
        shared.start()
        return shared

    rings["gate1"].finish()
    rings["lift1"].finish()
    exchange = unit_open(section, gains[0:1], gate1_all, lift1_all, rs1_src, rs1_dst)

    rings["drop1"].relay(2)
    rings["mix"].relay(1)
    rings["proj"].relay(1)
    gather = unit_hidden(exchange, rs1_dst, h1_all)

    rings["drop1"].relay(3)
    rings["gate2"].start()
    rings["lift2"].start()
    rings["mix"].relay(2)
    rings["proj"].relay(2)

    lane16 = lanes((16, 128))
    live = lane16 < lengths_ref[...] - 1
    masked = jnp.where(live, decay_ref[...], 0.0)
    later = (lax.broadcasted_iota(jnp.int32, (128, 128), 0) > lanes((128, 128))).astype(F32)
    tail = jnp.dot(masked, later, precision=HIGHEST, preferred_element_type=F32)
    decay_total = jnp.sum(masked, axis=1, keepdims=True)
    fading = jnp.where(live, jnp.exp(tail) * steps_ref[...], 0.0)

    def earlier(past_ref, taps_ref):
        rows = [
            jnp.sum(past_ref[s].astype(F32) * taps_ref[0:3, :], axis=0, keepdims=True)
            for s in range(OWN)
        ]
        return jnp.concatenate(rows, axis=0)

    value_earlier = earlier(value_past_ref, value_taps_ref)
    key_earlier = earlier(key_past_ref, key_taps_ref)
    query_earlier = earlier(query_past_ref, query_taps_ref)

    rings["drop1"].finish()
    shared = share(down(gather, h1_all, drop1_all, HIDP), sum1_all)
    rings["drop2"].start()
    rings["mix"].relay(3)
    rings["proj"].relay(3)
    shared.wait()
    section = (section + 0.5 * total(sum1_all)).astype(BF16).astype(F32)

    rings["mix"].finish()
    scaled = (section * gains[1:2]).astype(BF16)
    mix = jnp.dot(scaled, mix_all[...].reshape(256, MIXW), preferred_element_type=F32)
    mix = with_squares(mix, section, STEP_AT + 32)
    for k in range(N):
        rsm_src[k] = mix[OWN * k : OWN * k + OWN].astype(BF16)
    exchange = group(rsm_src, rsm_dst, 1, True)
    exchange.start()
    rsm_dst[y] = rsm_src[y]
    for name in ("gate2", "lift2", "drop2"):
        rings[name].relay(1)
    exchange.wait()
    summed = total(rsm_dst)
    summed = summed * row_scale(summed, STEP_AT + 32)
    new_value = silu(value_earlier + value_taps_ref[3:4, :] * summed[:, 0:256])
    gate_vals = silu(summed[:, 256:512])
    new_key = silu(key_earlier + key_taps_ref[3:4, :] * summed[:, 512:640])
    new_query = silu(query_earlier + query_taps_ref[3:4, :] * summed[:, 640:768])
    step_all = softplus(summed[:, 768:896])
    lane4 = lanes((OWN, 128))
    step = [
        jnp.sum(jnp.where(lane4 == OWN * t + j, step_all, 0.0), axis=1, keepdims=True)
        for j in range(4)
    ]
    fall = [-rate_ref[j] * step[j] for j in range(4)]
    self_score = jnp.sum(new_query * new_key, axis=1, keepdims=True)
    query8 = jnp.concatenate([new_query, jnp.zeros((OWN, 128), F32)], axis=0)
    query8_round = query8.astype(BF16)
    head_of = lanes((4, 256)) // 64
    own_head = head_of == lax.broadcasted_iota(jnp.int32, (4, 256), 0)
    rows = []
    for s in range(OWN):
        this_fall = jnp.concatenate([fall[j][s : s + 1] for j in range(4)], axis=0)
        this_step = jnp.concatenate([step[j][s : s + 1] for j in range(4)], axis=0)
        scores = dot_nt(query8_round, keys_ref[s])[s : s + 1]
        weights = (fading[4 * s : 4 * s + 4] * jnp.exp(this_fall) * scores).astype(BF16)
        weights8 = jnp.concatenate([weights.astype(F32), jnp.zeros((4, 128), F32)], axis=0)
        from_block = jnp.dot(
            weights8.astype(BF16), values_ref[s], preferred_element_type=F32
        )[0:4]
        from_state = dot_nt(query8, state_ref[s].reshape(256, 128), HIGHEST)[s : s + 1]
        from_state = jnp.exp(decay_total[4 * s : 4 * s + 4] + this_fall) * from_state
        from_token = (this_step * self_score[s : s + 1]) * new_value[s : s + 1]
        heads = from_state + from_block + from_token
        rows.append(jnp.sum(jnp.where(own_head, heads, 0.0), axis=0, keepdims=True))
    gated = jnp.concatenate(rows, axis=0) * gate_vals
    squares = gated * gated
    inverse = jnp.zeros((OWN, 256), F32)
    for j in range(4):
        mean = jnp.sum(jnp.where(head_of == j, squares, 0.0), axis=1, keepdims=True) / 64
        inverse = jnp.where(head_of == j, lax.rsqrt(mean + EPSILON), inverse)
    hm_all[y] = (gated * inverse * head_gain_ref[...]).astype(BF16)
    gather = group(hm_all, hm_all, 1, False)
    gather.start()
    for name in ("gate2", "lift2", "drop2"):
        rings[name].relay(2)
    rings["proj"].finish()
    shared = share(down(gather, hm_all, proj_all, 256), summ_all)
    for name in ("gate2", "lift2", "drop2"):
        rings[name].relay(3)
    shared.wait()
    section = (section + total(summ_all)).astype(BF16).astype(F32)

    rings["gate2"].finish()
    rings["lift2"].finish()
    exchange = unit_open(section, gains[2:3], gate2_all, lift2_all, rs2_src, rs2_dst)

    for k in range(N):
        two_src[k] = piece(section, k).astype(BF16)
    two_copy = pltpu.make_async_remote_copy(
        src_ref=two_src.at[t],
        dst_ref=two_dst,
        send_sem=two_send,
        recv_sem=two_recv,
        device_id=at(t, y, z),
        device_id_type=MESH,
    )

    @pl.when(jnp.logical_not(diagonal))
    def _():
        two_copy.start()

    @pl.when(diagonal)
    def _():
        two_dst[...] = two_src[t]

    gather = unit_hidden(exchange, rs2_dst, h2_all)
    rings["drop2"].finish()
    part = down(gather, h2_all, drop2_all, HIDP)
    for k in range(N):
        end_src[k] = piece(part, k).astype(BF16)

    def end_copy(d):
        to = plus(z, d)
        return pltpu.make_async_remote_copy(
            src_ref=end_src.at[to],
            dst_ref=end_dst.at[t],
            send_sem=end_send.at[d],
            recv_sem=end_recv.at[t],
            device_id=at(to, y, z),
            device_id_type=MESH,
        )

    def end_start(d, c):
        end_copy(d).start()
        return c

    lax.fori_loop(1, N, end_start, 0)

    @pl.when(jnp.logical_not(diagonal))
    def _():
        end_copy(0).start()

    @pl.when(diagonal)
    def _():
        end_dst[t] = end_src[z]

    def end_wait(k):
        return pltpu.make_async_remote_copy(
            src_ref=end_dst.at[k],
            dst_ref=end_dst.at[k],
            send_sem=end_send.at[0],
            recv_sem=end_recv.at[k],
            device_id=me,
            device_id_type=MESH,
        )

    for each in groups:
        each.drain()
    for each in rings.values():
        each.drain()

    def x_drain(d, c):
        x_copy(d).wait_send()
        return c

    lax.fori_loop(1, N, x_drain, 0)

    @pl.when(jnp.logical_not(diagonal))
    def _():
        x_copy(0).wait_send()
        two_copy.wait_send()
        two_copy.wait_recv()

    def end_arrived(d, c):
        end_wait(plus(t, d)).wait_recv()
        return c

    lax.fori_loop(1, N, end_arrived, 0)

    @pl.when(jnp.logical_not(diagonal))
    def _():
        end_wait(t).wait_recv()

    result = two_dst[...].astype(F32) + 0.5 * total(end_dst)
    out_ref[...] = result[:, 0:32].astype(BF16)

    def end_drain(d, c):
        end_copy(d).wait_send()
        return c

    lax.fori_loop(1, N, end_drain, 0)

    @pl.when(jnp.logical_not(diagonal))
    def _():
        end_copy(0).wait_send()


def on_device(
    hidden_in,
    gain_before,
    gate_before,
    lift_before,
    drop_before,
    mixer_gain,
    value_proj,
    gate_proj,
    key_proj,
    query_proj,
    step_proj,
    value_taps,
    key_taps,
    query_taps,
    value_past,
    key_past,
    query_past,
    decay_rate,
    block_state,
    block_keys,
    block_values,
    block_steps,
    block_decay,
    lengths,
    head_gain,
    out_proj,
    gain_after,
    gate_after,
    lift_after,
    drop_after,
):
    gains = jnp.pad(jnp.stack([gain_before, mixer_gain, gain_after]), ((0, 5), (0, 96)))
    by_head = lambda a: jnp.swapaxes(a, 1, 2).reshape(16, 128)
    args = (
        hidden_in,
        gains,
        gate_before,
        lift_before,
        drop_before,
        value_proj,
        gate_proj,
        key_proj,
        query_proj,
        step_proj,
        value_taps,
        key_taps,
        query_taps,
        value_past,
        key_past,
        query_past,
        decay_rate,
        block_state,
        block_keys,
        block_values,
        by_head(block_steps),
        by_head(block_decay),
        jnp.repeat(lengths, 4)[:, None],
        head_gain[None, :],
        out_proj,
        gate_after,
        lift_after,
        drop_after,
    )
    vmem = pl.BlockSpec(memory_space=pltpu.VMEM)
    smem = pl.BlockSpec(memory_space=pltpu.SMEM)
    wide = pltpu.VMEM((N, ROWS, HIDP), BF16)
    scratch = [
        pltpu.VMEM((ROWS, 128), BF16),
        pltpu.VMEM((N, ROWS, 128), BF16),
        pltpu.VMEM((N, 8, 128), F32),
        wide,
        wide,
        wide,
        pltpu.VMEM((N, ROWS, MIXW), BF16),
        pltpu.VMEM((N, ROWS, 256), BF16),
        wide,
        wide,
        wide,
        pltpu.VMEM((N, OWN, 2 * HIDP), BF16),
        pltpu.VMEM((N, OWN, 2 * HIDP), BF16),
        pltpu.VMEM((N, OWN, HIDP), BF16),
        pltpu.VMEM((N, ROWS, 256), BF16),
        pltpu.VMEM((N, OWN, MIXW), BF16),
        pltpu.VMEM((N, OWN, MIXW), BF16),
        pltpu.VMEM((N, OWN, 256), BF16),
        pltpu.VMEM((N, ROWS, 256), BF16),
        pltpu.VMEM((N, OWN, 2 * HIDP), BF16),
        pltpu.VMEM((N, OWN, 2 * HIDP), BF16),
        pltpu.VMEM((N, OWN, HIDP), BF16),
        pltpu.VMEM((N, ROWS, 128), BF16),
        pltpu.VMEM((ROWS, 128), BF16),
        pltpu.VMEM((N, ROWS, 128), BF16),
        pltpu.VMEM((N, ROWS, 128), BF16),
        pltpu.SemaphoreType.DMA((9, 4)),
        pltpu.SemaphoreType.DMA((9, 3)),
        pltpu.SemaphoreType.DMA((9, N)),
        pltpu.SemaphoreType.DMA((8, N)),
        pltpu.SemaphoreType.DMA((8, N)),
        pltpu.SemaphoreType.DMA((N,)),
        pltpu.SemaphoreType.DMA((N,)),
        pltpu.SemaphoreType.DMA((N,)),
        pltpu.SemaphoreType.DMA((N,)),
        pltpu.SemaphoreType.DMA,
        pltpu.SemaphoreType.DMA,
    ]
    return pl.pallas_call(
        kernel,
        out_shape=jax.ShapeDtypeStruct((ROWS, 32), BF16),
        in_specs=[smem if k == 16 else vmem for k in range(len(args))],
        out_specs=vmem,
        scratch_shapes=scratch,
        compiler_params=pltpu.CompilerParams(collective_id=0, has_side_effects=True),
    )(*args)


def solution(mesh):
    finer = Mesh(mesh.devices.reshape(N, N, N), ("z", "y", "t"))
    kv = ("z", "y")
    return jax.shard_map(
        on_device,
        mesh=finer,
        in_specs=(
            P("t", kv),
            P(kv),
            P(kv, "t"),
            P(kv, "t"),
            P("t", kv),
            P(kv),
            P(kv, "t"),
            P(kv, "t"),
            P(kv, "t"),
            P(kv, "t"),
            P(kv, None),
            P(None, "t"),
            P(None, "t"),
            P(None, "t"),
            P(kv, None, "t"),
            P(kv, None, "t"),
            P(kv, None, "t"),
            P("t"),
            P(kv, "t", None, None),
            P(kv, None, "t"),
            P(kv, None, "t"),
            P(kv, None, "t"),
            P(kv, None, "t"),
            P(kv),
            P("t"),
            P("t", kv),
            P(kv),
            P(kv, "t"),
            P(kv, "t"),
            P("t", kv),
        ),
        out_specs=P("t", kv),
        check_vma=False,
    )
```
